32 devices in a mesh: sp: 8 (over z, y), tp: 4 (over x, core).
Axes of the slice: x: 2, y: 2, z: 4, core: 2. Of those that a mesh axis runs over, the one named last changes fastest.
Arguments:
- residual_entry_input: bfloat16 [8192, 2048], P(('sp', 'tp')), may hold values from -6 to 6
- query_matrix_rows: bfloat16 [8192, 1024], P('sp', 'tp'), may hold values from -6 to 6
- key_matrix_rows: bfloat16 [8192, 1024], P('sp', 'tp'), may hold values from -6 to 6
- value_matrix_rows: bfloat16 [8192, 2048], P('sp', 'tp'), may hold values from -6 to 6
- output_gate_logits: bfloat16 [8192, 2048], P('sp', 'tp'), may hold values from -6 to 6
- input_gate_logits: float32 [8192, 8], P('sp', 'tp'), may hold values from -6 to 6
- forget_gate_logits: float32 [8192, 8], P('sp', 'tp'), may hold values from -8 to 31
- forget_decay_offset: float32 [8192, 8], P('sp', 'tp'), may hold values from -0.7 to 0
- head_norm_gain: float32 [8, 256], P('tp'), may hold values from 0.1 to 1.9
- cell_output_weight: bfloat16 [2048, 2048], P('tp'), may hold values from -0.125 to 0.125
- feedforward_norm_gain: float32 [2048], replicated, may hold values from 0.1 to 1.9
- gate_up_weight: bfloat16 [2048, 5632], P('sp', 'tp'), may hold values from -0.125 to 0.125
- value_up_weight: bfloat16 [2048, 5632], P('sp', 'tp'), may hold values from -0.125 to 0.125
- gate_filter_taps: float32 [3, 5632], P(None, 'tp'), may hold values from -3 to 3
- value_filter_taps: float32 [3, 5632], P(None, 'tp'), may hold values from -3 to 3
- down_projection_weight: bfloat16 [5632, 2048], P('tp', 'sp'), may hold values from -0.078125 to 0.078125
Outputs:
- result: bfloat16 [8192, 2048], P(('sp', 'tp'))
The draws below stay inside these ranges and needn't reach their ends.
All inputs are finite; a program needn't handle non-finite values.
Results may differ from the reference program's by a relative error of at most 0.025.
Values may be sent and summed in bfloat16 or wider, within the bound.
A program may use at most 128 MiB of HBM per device.

```python
import math
import jax
import jax.numpy as jnp
from jax import lax

D = 2048
HEADS = 8
DK = 128
DV = 256
FF = 5632
BLOCK = 128
TOK_DEV = 1024
TOKENS = 8192
HV = 2048
FF_DEV = 1408
N_TP = 4


def draw_forget_gate_logits(key, part):
    key_order = jax.random.fold_in(key, 11)
    key_slow = jax.random.fold_in(key, 12)
    key_fast = jax.random.fold_in(key, 13)
    key_noise = jax.random.fold_in(key, 14)
    order = jax.random.permutation(key_order, HEADS)
    slow_heads = order < HEADS // 2
    slow_rate = math.log(10.0) / (6.0 * TOKENS) * jnp.exp(jax.random.uniform(key_slow, (HEADS,), jnp.float32, math.log(0.5), 0.0))
    fast_rate = 1.0 / 40.0 * jnp.exp(jax.random.uniform(key_fast, (HEADS,), jnp.float32, math.log(0.6), math.log(1.6)))
    head_rate = jnp.where(slow_heads, slow_rate, fast_rate)
    block_index = jnp.arange(TOKENS) // TOK_DEV
    device_factor = (1 + block_index % 2).astype(jnp.float32)
    noise = jnp.clip(jax.random.normal(key_noise, (TOKENS, HEADS), jnp.float32), -4.0, 4.0)
    rate = head_rate[None, :] * device_factor[:, None] * jnp.exp(0.7 * noise)
    capped = jnp.clip(-jnp.log(jnp.expm1(rate)), -6.0, 14.5)
    ratio = capped / 15.0
    return (7.5 * jnp.log((1.0 + ratio) / (1.0 - ratio))).astype(jnp.float32)


def draw_forget_decay_offset(key, part):
    key_where = jax.random.fold_in(key, 21)
    key_depth = jax.random.fold_in(key, 22)
    spots = jax.random.randint(key_where, (2,), 0, TOKENS)
    depth = jax.random.uniform(key_depth, (2, HEADS), jnp.float32, math.log(0.5), math.log(0.8))
    positions = jnp.arange(TOKENS)
    first = jnp.where((positions == spots[0])[:, None], depth[0][None, :], 0.0)
    second = jnp.where((positions == spots[1])[:, None], depth[1][None, :], 0.0)
    return (first + second).astype(jnp.float32)


def steps_of(rng, extent, split, low, top_value):
    def one(axis_at, blocks):
        draws = jax.random.uniform(jax.random.fold_in(jax.random.fold_in(rng, 6), axis_at), (blocks,), jnp.float32, low / len(split), top_value / len(split))
        return jnp.repeat(jnp.exp(draws), extent[axis_at] // blocks).reshape((-1,) + (1,) * (len(extent) - axis_at - 1))

    factor_of = one(*split[0])
    for cut in split[1:]:
        factor_of = factor_of * one(*cut)
    return factor_of


def normal_values(own_key, dims, width, most, cuts=(), kind=jnp.bfloat16):
    array = width * jax.random.normal(own_key, dims, jnp.float32)
    if cuts:
        array = array * steps_of(own_key, dims, cuts, -0.22, 0.18)
    return jnp.clip(array, -most, most).astype(kind)


def setup_inputs(seed: int = 0) -> dict:
    keys = jax.random.split(jax.random.key(seed), 17)
    return {
        "residual_entry_input": normal_values(keys[0], (TOKENS, D), 1.0, 6.0, ((0, 32),)),
        "query_matrix_rows": normal_values(keys[1], (TOKENS, HEADS * DK), 1.0, 6.0, ((0, 8), (1, 4))),
        "key_matrix_rows": normal_values(keys[2], (TOKENS, HEADS * DK), 1.0, 6.0, ((0, 8), (1, 4))),
        "value_matrix_rows": normal_values(keys[3], (TOKENS, HV), 1.0, 6.0, ((0, 8), (1, 4))),
        "output_gate_logits": normal_values(keys[4], (TOKENS, HV), 1.0, 6.0, ((0, 8), (1, 4))),
        "input_gate_logits": normal_values(keys[5], (TOKENS, HEADS), 1.0, 6.0, ((0, 8), (1, 4)), jnp.float32),
        "forget_gate_logits": draw_forget_gate_logits(jax.random.fold_in(keys[16], 71), 0),
        "forget_decay_offset": draw_forget_decay_offset(jax.random.fold_in(keys[16], 71), 0),
        "head_norm_gain": jnp.clip(1.0 + 0.18 * jax.random.normal(keys[8], (HEADS, DV), jnp.float32), 0.1, 1.9),
        "cell_output_weight": normal_values(keys[9], (HV, D), HV ** -0.5, 0.125, ((0, 4),)),
        "feedforward_norm_gain": jnp.clip(1.0 + 0.18 * jax.random.normal(keys[10], (D,), jnp.float32), 0.1, 1.9),
        "gate_up_weight": normal_values(keys[11], (D, FF), D ** -0.5, 0.125, ((0, 8), (1, 4))),
        "value_up_weight": normal_values(keys[12], (D, FF), D ** -0.5, 0.125, ((0, 8), (1, 4))),
        "gate_filter_taps": normal_values(keys[13], (3, FF), 0.577, 3.0, ((1, 4),), jnp.float32),
        "value_filter_taps": normal_values(keys[14], (3, FF), 0.577, 3.0, ((1, 4),), jnp.float32),
        "down_projection_weight": normal_values(keys[15], (FF, D), FF ** -0.5, 0.078125, ((0, 4), (1, 8))),
    }


eps = 1e-06

def gate_log_values(input_gate_logits, forget_gate_logits, forget_decay_offset):
    input_log_value = 15.0 * jnp.tanh(input_gate_logits / 15.0)
    forget_log_sigmoid = jax.nn.log_sigmoid(15.0 * jnp.tanh(forget_gate_logits / 15.0)) + forget_decay_offset
    return (input_log_value, forget_log_sigmoid)

def block_step(state_carry, inputs):
    memory, normer, running = state_carry
    query_block, key_block, value_block, input_block, forget_block = inputs
    length = query_block.shape[0]
    highest = lax.Precision.HIGHEST
    query_scale = DK ** (-0.5)
    query_wide = query_block.astype(jnp.float32)
    key_wide = key_block.astype(jnp.float32)
    value_wide = value_block.astype(jnp.float32)
    causal = jnp.tril(jnp.ones((length, length), dtype=bool))[:, :, None]
    cumulative = jnp.cumsum(forget_block, axis=0)
    logits = cumulative[:, None, :] - cumulative[None, :, :] + input_block[None, :, :]
    logits = jnp.where(causal, logits, -jnp.inf)
    carried = cumulative + running[None, :]
    stable = jnp.maximum(carried, lax.optimization_barrier(jnp.max(logits, axis=1)))
    carry_weight = jnp.exp(carried - stable)
    raw = jnp.einsum('thd,shd->tsh', query_wide, key_wide) * query_scale
    scores = raw * jnp.exp(logits - stable[:, None, :])
    scores_low = scores.astype(jnp.bfloat16).astype(jnp.float32)
    scaled_query = query_wide * query_scale
    numerator = carry_weight[:, :, None] * jnp.einsum('hvd,thd->thv', memory, scaled_query, precision=highest)
    numerator = numerator + jnp.einsum('tsh,shv->thv', scores_low, value_wide)
    denominator = carry_weight * jnp.einsum('hd,thd->th', normer, scaled_query, precision=highest) + lax.optimization_barrier(jnp.sum(scores, axis=1))
    output = numerator / jnp.maximum(jnp.abs(denominator), jnp.exp(-stable))[:, :, None]
    last_sum = cumulative[-1]
    weights_log = last_sum[None, :] - cumulative + input_block
    new_running = jnp.maximum(last_sum + running, lax.optimization_barrier(jnp.max(weights_log, axis=0)))
    decay_factor = jnp.exp(last_sum + running - new_running)
    weighted = key_wide * jnp.exp(weights_log - new_running[None, :])[:, :, None]
    weighted_low = weighted.astype(jnp.bfloat16).astype(jnp.float32)
    memory = decay_factor[:, None, None] * memory + jnp.einsum('shv,shd->hvd', value_wide, weighted_low)
    normer = decay_factor[:, None] * normer + lax.optimization_barrier(jnp.sum(weighted, axis=0))
    return ((memory, normer, new_running), output)

def reference(residual_entry_input, query_matrix_rows, key_matrix_rows, value_matrix_rows, output_gate_logits, input_gate_logits, forget_gate_logits, forget_decay_offset, head_norm_gain, cell_output_weight, feedforward_norm_gain, gate_up_weight, value_up_weight, gate_filter_taps, value_filter_taps, down_projection_weight):
    token_count = query_matrix_rows.shape[0]
    queries = query_matrix_rows.reshape(token_count, HEADS, DK)
    keys_all = key_matrix_rows.reshape(token_count, HEADS, DK)
    values_all = value_matrix_rows.reshape(token_count, HEADS, DV)
    input_log_value, forget_log_sigmoid = gate_log_values(input_gate_logits, forget_gate_logits, forget_decay_offset)
    block_count = token_count // BLOCK

    def blocks(tensor):
        return tensor.reshape((block_count, BLOCK) + tensor.shape[1:])
    initial = (jnp.zeros((HEADS, DV, DK), jnp.float32), jnp.zeros((HEADS, DK), jnp.float32), jnp.zeros((HEADS,), jnp.float32))
    _, outputs = lax.scan(block_step, initial, (blocks(queries), blocks(keys_all), blocks(values_all), blocks(input_log_value), blocks(forget_log_sigmoid)))
    memory_out = outputs.reshape(token_count, HEADS, DV)
    normed = memory_out * lax.rsqrt(lax.optimization_barrier(jnp.mean(memory_out * memory_out, axis=-1, keepdims=True)) + eps) * head_norm_gain[None, :, :]
    gated_rows = (normed.reshape(token_count, HEADS * DV) * jax.nn.sigmoid(output_gate_logits.astype(jnp.float32))).astype(jnp.bfloat16)
    mixed_rows = jnp.dot(gated_rows, cell_output_weight, preferred_element_type=jnp.float32)
    stream = (residual_entry_input.astype(jnp.float32) + mixed_rows).astype(jnp.bfloat16)
    stream_wide = lax.optimization_barrier(stream).astype(jnp.float32)
    normed_rows = (stream_wide * lax.rsqrt(lax.optimization_barrier(jnp.mean(stream_wide * stream_wide, axis=-1, keepdims=True)) + eps) * feedforward_norm_gain[None, :]).astype(jnp.bfloat16)
    padded = jnp.concatenate([jnp.zeros((2, D), jnp.bfloat16), normed_rows], axis=0)
    row_block = min(token_count, 4096)
    pieces = []
    for offset in range(0, token_count, row_block):
        window = padded[offset:offset + row_block + 2]
        up_gate = jnp.dot(window, gate_up_weight, preferred_element_type=jnp.float32)
        up_value = jnp.dot(window, value_up_weight, preferred_element_type=jnp.float32)
        conv_g = gate_filter_taps[0][None, :] * up_gate[:-2] + gate_filter_taps[1][None, :] * up_gate[1:-1] + gate_filter_taps[2][None, :] * up_gate[2:]
        conv_v = value_filter_taps[0][None, :] * up_value[:-2] + value_filter_taps[1][None, :] * up_value[1:-1] + value_filter_taps[2][None, :] * up_value[2:]
        hidden = (jax.nn.silu(conv_g) * conv_v).astype(jnp.bfloat16)
        running_sum = jnp.zeros((row_block, D), jnp.float32)
        for member in range(N_TP):
            lower = member * FF_DEV
            partial_value = jnp.dot(hidden[:, lower:lower + FF_DEV], down_projection_weight[lower:lower + FF_DEV], preferred_element_type=jnp.float32).astype(jnp.bfloat16)
            running_sum = running_sum + lax.optimization_barrier(partial_value).astype(jnp.float32)
        pieces.append((stream_wide[offset:offset + row_block] + running_sum).astype(jnp.bfloat16))
    return jnp.concatenate(pieces, axis=0)
```

```python
import functools

import jax
import jax.numpy as jnp
from jax import lax
from jax.experimental import pallas as pl
from jax.experimental.pallas import tpu as pltpu
from jax.sharding import PartitionSpec as P

BLOCK = 128


eps = 1e-06
neg_large = -1e30


def shifted(x, axis, by):
    count = lax.axis_size(axis)
    pairs = [(i, i + by) for i in range(count) if 0 <= i + by < count]
    return lax.ppermute(x, axis, pairs)


def gate_log_values(input_gate_logits, forget_gate_logits, forget_decay_offset):
    input_log_value = 15.0 * jnp.tanh(input_gate_logits / 15.0)
    forget_log_sigmoid = (
        jax.nn.log_sigmoid(15.0 * jnp.tanh(forget_gate_logits / 15.0)) + forget_decay_offset
    )
    return (input_log_value, forget_log_sigmoid)


STATE_PAD = 16
MESH = pl.DeviceIdType.MESH


def cell_kernel(
    count,
    heads,
    state_ref,
    q_ref,
    k_ref,
    v_ref,
    gate_ref,
    gain_ref,
    rows_ref,
    cols_ref,
    out_ref,
    held,
    memory,
    normer,
    running,
    send_sem,
    recv_sem,
):
    me = lax.axis_index("sp")
    barrier = pltpu.get_barrier_semaphore()
    for d in range(1, count):
        pl.semaphore_signal(
            barrier, inc=1, device_id={"sp": lax.rem(me + d, count)}, device_id_type=MESH
        )
    pl.semaphore_wait(barrier, count - 1)

    def push(d, target, slot):
        return pltpu.make_async_remote_copy(
            src_ref=state_ref,
            dst_ref=held.at[slot],
            send_sem=send_sem.at[d],
            recv_sem=recv_sem.at[d],
            device_id={"sp": target},
            device_id_type=MESH,
        )

    for d in range(1, count):

        @pl.when(me + d < count)
        def _():
            push(d, me + d, me).start()

    memory[...] = jnp.zeros_like(memory)
    normer[...] = jnp.zeros_like(normer)
    running[...] = jnp.full(running.shape, neg_large, jnp.float32)
    for d in range(1, count):

        @pl.when(me - d >= 0)
        def _():
            push(d, lax.rem(me + d, count), me - d).wait_recv()

    key_width = memory.shape[1]
    value_width = memory.shape[2]
    span = key_width + STATE_PAD

    @pl.loop(0, me)
    def _(j):
        for h in range(heads):
            low = h * span
            extra = held[j, low + key_width : low + span, :].astype(jnp.float32)
            total = extra[2:3, :1] + extra[3:4, :1]
            level = extra[4:5, :1] + extra[5:6, :1]
            before = running[h, :1, :1]
            after = jnp.maximum(total + before, level)
            one = jnp.exp(total + before - after)
            two = jnp.exp(level - after)
            memory[h] = one * memory[h] + two * held[j, low : low + key_width, :].astype(
                jnp.float32
            )
            parts = extra[0:1, :key_width] + extra[1:2, :key_width]
            normer[h, :1, :] = one * normer[h, :1, :] + two * parts
            running[h] = jnp.broadcast_to(after, running.shape[1:])

    length = BLOCK
    scale = key_width ** (-0.5)
    at_row = lax.broadcasted_iota(jnp.int32, (length, length), 0)
    at_col = lax.broadcasted_iota(jnp.int32, (length, length), 1)
    causal = at_col <= at_row

    @pl.loop(0, q_ref.shape[0] // length)
    def _(j):
        rows = pl.ds(pl.multiple_of(j * length, length), length)
        lanes = rows_ref[j]
        cols = cols_ref[rows, :]
        for h in range(heads):
            keys = slice(h * key_width, (h + 1) * key_width)
            vals = slice(h * value_width, (h + 1) * value_width)
            q = q_ref[rows, keys]
            k = k_ref[rows, keys]
            v = v_ref[rows, vals]
            before = running[h, :1, :1]
            total = lanes[heads + h : heads + h + 1, :1]
            shifted_log = jnp.where(causal, lanes[h : h + 1, :], -jnp.inf)
            top = jnp.maximum(jnp.max(shifted_log, axis=1, keepdims=True), before)
            raw = (
                lax.dot_general(
                    q, k, (((1,), (1,)), ((), ())), preferred_element_type=jnp.float32
                )
                * scale
            )
            scores = raw * jnp.exp(shifted_log - top)
            carry = jnp.exp(before - top) * scale
            state = memory[h]
            high = state.astype(jnp.bfloat16)
            low = (state - high.astype(jnp.float32)).astype(jnp.bfloat16)
            carried = jnp.dot(q, high, preferred_element_type=jnp.float32) + jnp.dot(
                q, low, preferred_element_type=jnp.float32
            )
            numerator = carry * carried + jnp.dot(
                scores.astype(jnp.bfloat16), v, preferred_element_type=jnp.float32
            )
            denominator = carry * jnp.sum(
                q.astype(jnp.float32) * normer[h, :1, :], axis=1, keepdims=True
            ) + jnp.sum(scores, axis=1, keepdims=True)
            level = cols[:, h : h + 1] + top
            value = numerator / jnp.maximum(jnp.abs(denominator), jnp.exp(-level))
            mean = jnp.mean(value * value, axis=1, keepdims=True)
            normed = value * lax.rsqrt(mean + eps) * gain_ref[h : h + 1, :]
            gated = normed * jax.nn.sigmoid(gate_ref[rows, vals].astype(jnp.float32))
            out_ref[rows, vals] = gated.astype(out_ref.dtype)
            last = jnp.max(jnp.maximum(lanes[h : h + 1, :], before), axis=1, keepdims=True)
            decay = jnp.exp(before - last)
            weighted = k.astype(jnp.float32) * jnp.exp(cols[:, heads + h : heads + h + 1] - last)
            memory[h] = decay * state + lax.dot_general(
                weighted.astype(jnp.bfloat16),
                v,
                (((0,), (0,)), ((), ())),
                preferred_element_type=jnp.float32,
            )
            normer[h, :1, :] = decay * normer[h, :1, :] + jnp.sum(
                weighted, axis=0, keepdims=True
            )
            running[h] = jnp.broadcast_to(last + total, running.shape[1:])

    for d in range(1, count):

        @pl.when(me + d < count)
        def _():
            push(d, me + d, me).wait_send()


def halves(x):
    high = lax.reduce_precision(x, 8, 7)
    return (high.astype(jnp.bfloat16), (x - high).astype(jnp.bfloat16))


def cell(q, k, v, gates, input_log, forget_log, gain):
    heads = input_log.shape[1]
    tokens = q.shape[0]
    key_width = q.shape[1] // heads
    value_width = v.shape[1] // heads
    count = lax.axis_size("sp")
    blocks = tokens // BLOCK
    f = forget_log.reshape(blocks, BLOCK, heads)
    tri = jnp.tril(jnp.ones((BLOCK, BLOCK), jnp.float32))
    within = jnp.einsum("ts,bsh->bth", tri, f, precision=lax.Precision.HIGHEST)
    each = within[:, -1, :]
    later = jnp.triu(jnp.ones((blocks, blocks), jnp.float32), 1)
    after = jnp.einsum("bc,ch->bh", later, each, precision=lax.Precision.HIGHEST)
    total = jnp.sum(each, axis=0)
    shifted_log = input_log.reshape(blocks, BLOCK, heads) - within
    to_end = (shifted_log + (each + after)[:, None, :]).reshape(tokens, heads)
    level = jnp.max(to_end, axis=0)
    weighted = k.reshape(tokens, heads, key_width).astype(jnp.float32) * jnp.exp(to_end - level)[
        :, :, None
    ]
    memory = jnp.einsum(
        "shd,shv->hdv",
        weighted.astype(jnp.bfloat16),
        v.reshape(tokens, heads, value_width),
        preferred_element_type=jnp.float32,
    ).astype(jnp.bfloat16)
    normer = jnp.sum(weighted, axis=0)
    wide = (heads, 1, value_width)
    lines = [
        jnp.pad(part, ((0, 0), (0, value_width - key_width)))[:, None, :]
        for part in halves(normer)
    ]
    for scalar in (total, level):
        lines += [jnp.broadcast_to(part[:, None, None], wide) for part in halves(scalar)]
    lines.append(jnp.zeros((heads, STATE_PAD - len(lines), value_width), jnp.bfloat16))
    span = key_width + STATE_PAD
    state = jnp.concatenate([memory] + lines, axis=1).reshape(heads * span, value_width)
    lanes = jnp.concatenate(
        [
            jnp.transpose(shifted_log, (0, 2, 1)),
            jnp.broadcast_to(each[:, :, None], (blocks, heads, BLOCK)),
        ],
        axis=1,
    )
    cols = jnp.concatenate([within, shifted_log], axis=2).reshape(tokens, 2 * heads)
    vmem = pl.BlockSpec(memory_space=pltpu.VMEM)
    return pl.pallas_call(
        functools.partial(cell_kernel, count, heads),
        out_shape=jax.ShapeDtypeStruct(v.shape, jnp.bfloat16),
        in_specs=[vmem] * 8,
        out_specs=vmem,
        scratch_shapes=[
            pltpu.VMEM((count, heads * span, value_width), jnp.bfloat16),
            pltpu.VMEM((heads, key_width, value_width), jnp.float32),
            pltpu.VMEM((heads, 8, key_width), jnp.float32),
            pltpu.VMEM((heads, 8, 128), jnp.float32),
            pltpu.SemaphoreType.DMA((count,)),
            pltpu.SemaphoreType.DMA((count,)),
        ],
        compiler_params=pltpu.CompilerParams(
            collective_id=0, has_side_effects=True, vmem_limit_bytes=40 * 1024 * 1024
        ),
        cost_estimate=pl.CostEstimate(
            flops=30_000_000_000, bytes_accessed=8 * v.size, transcendentals=0
        ),
    )(state, q, k, v, gates, gain, lanes, cols)


def rows_kernel(pieces, x_ref, out_ref, own_sem, near_send, near_recv, far_send, far_recv, on_send, on_recv):
    me = lax.axis_index("tp")
    near = me + 1 - 2 * lax.rem(me, 2)
    far = lax.rem(me + 2, 4)
    opposite = lax.rem(near + 2, 4)
    size = x_ref.shape[0]
    step = size // pieces
    barrier = pltpu.get_barrier_semaphore()
    for other in (near, far):
        pl.semaphore_signal(barrier, inc=1, device_id={"tp": other}, device_id_type=MESH)
    pl.semaphore_wait(barrier, 2)

    def at(owner, p):
        return out_ref.at[pl.ds(pl.multiple_of(owner * size + p * step, step), step)]

    def send(src, dst, sems, p, target):
        return pltpu.make_async_remote_copy(
            src_ref=src,
            dst_ref=dst,
            send_sem=sems[0].at[p],
            recv_sem=sems[1].at[p],
            device_id={"tp": target},
            device_id_type=MESH,
        )

    mine = [x_ref.at[pl.ds(p * step, step)] for p in range(pieces)]
    far_out = [send(mine[p], at(me, p), (far_send, far_recv), p, far) for p in range(pieces)]
    near_out = [send(mine[p], at(me, p), (near_send, near_recv), p, near) for p in range(pieces)]
    far_in = [send(mine[p], at(far, p), (far_send, far_recv), p, far) for p in range(pieces)]
    near_in = [send(mine[p], at(near, p), (near_send, near_recv), p, near) for p in range(pieces)]
    onward = [send(at(far, p), at(far, p), (on_send, on_recv), p, near) for p in range(pieces)]
    on_in = [
        send(at(opposite, p), at(opposite, p), (on_send, on_recv), p, near)
        for p in range(pieces)
    ]
    for p in range(pieces):
        far_out[p].start()
    for p in range(pieces):
        near_out[p].start()
    whole = pl.ds(pl.multiple_of(me * size, size), size)
    own = pltpu.make_async_copy(x_ref, out_ref.at[whole], own_sem)
    own.start()
    for p in range(pieces):
        far_in[p].wait_recv()
        onward[p].start()
    own.wait()
    for p in range(pieces):
        near_in[p].wait_recv()
        on_in[p].wait_recv()
    for p in range(pieces):
        far_out[p].wait_send()
        near_out[p].wait_send()
        onward[p].wait_send()


def gather_rows(x):
    if lax.axis_size("tp") != 4:
        return lax.all_gather(x, "tp", axis=0, tiled=True)
    pieces = 4
    vmem = pl.BlockSpec(memory_space=pltpu.VMEM)
    return pl.pallas_call(
        functools.partial(rows_kernel, pieces),
        out_shape=jax.ShapeDtypeStruct((4 * x.shape[0], x.shape[1]), x.dtype),
        in_specs=[vmem],
        out_specs=vmem,
        scratch_shapes=[pltpu.SemaphoreType.DMA] + [pltpu.SemaphoreType.DMA((pieces,))] * 6,
        compiler_params=pltpu.CompilerParams(
            collective_id=1, has_side_effects=True, vmem_limit_bytes=16 * 1024 * 1024
        ),
        cost_estimate=pl.CostEstimate(
            flops=30_000_000_000, bytes_accessed=4 * x.size, transcendentals=0
        ),
    )(x)


def local(
    residual_entry_input,
    query_matrix_rows,
    key_matrix_rows,
    value_matrix_rows,
    output_gate_logits,
    input_gate_logits,
    forget_gate_logits,
    forget_decay_offset,
    head_norm_gain,
    cell_output_weight,
    feedforward_norm_gain,
    gate_up_weight,
    value_up_weight,
    gate_filter_taps,
    value_filter_taps,
    down_projection_weight,
):
    input_log, forget_log = gate_log_values(
        input_gate_logits, forget_gate_logits, forget_decay_offset
    )
    whole_gate = lax.all_gather(gate_up_weight, "sp", axis=0, tiled=True)
    whole_value = lax.all_gather(value_up_weight, "sp", axis=0, tiled=True)
    whole_down = lax.all_gather(down_projection_weight, "sp", axis=1, tiled=True)
    gated_rows = cell(
        query_matrix_rows,
        key_matrix_rows,
        value_matrix_rows,
        output_gate_logits,
        input_log,
        forget_log,
        head_norm_gain,
    )
    whole_out = lax.all_gather(cell_output_weight, "tp", axis=0, tiled=True)
    own_rows = lax.all_to_all(gated_rows, "tp", split_axis=0, concat_axis=1, tiled=True)
    mixed_rows = jnp.dot(own_rows, whole_out, preferred_element_type=jnp.float32)
    stream_wide = residual_entry_input.astype(jnp.float32) + mixed_rows
    stream = stream_wide.astype(jnp.bfloat16)
    stream_wide = lax.optimization_barrier(stream).astype(jnp.float32)
    normed_rows = (
        stream_wide
        * lax.rsqrt(jnp.mean(stream_wide * stream_wide, axis=-1, keepdims=True) + eps)
        * feedforward_norm_gain[None, :]
    ).astype(jnp.bfloat16)
    group_rows = gather_rows(normed_rows)
    earlier_rows = shifted(group_rows[-2:], "sp", 1)
    window = jnp.concatenate([earlier_rows, group_rows], axis=0)
    up_gate = jnp.dot(
        window,
        whole_gate,
        preferred_element_type=jnp.float32,
    )
    up_value = jnp.dot(
        window,
        whole_value,
        preferred_element_type=jnp.float32,
    )
    conv_g = (
        gate_filter_taps[0][None, :] * up_gate[:-2]
        + gate_filter_taps[1][None, :] * up_gate[1:-1]
        + gate_filter_taps[2][None, :] * up_gate[2:]
    )
    conv_v = (
        value_filter_taps[0][None, :] * up_value[:-2]
        + value_filter_taps[1][None, :] * up_value[1:-1]
        + value_filter_taps[2][None, :] * up_value[2:]
    )
    hidden = (jax.nn.silu(conv_g) * conv_v).astype(jnp.bfloat16)
    ffn_rows = lax.psum_scatter(
        jnp.dot(hidden, whole_down, preferred_element_type=jnp.float32).astype(jnp.bfloat16),
        "tp",
        scatter_dimension=0,
        tiled=True,
    ).astype(jnp.float32)
    return (stream_wide + ffn_rows).astype(jnp.bfloat16)


def solution(mesh):
    in_specs = (
        P(("sp", "tp"), None),
        P("sp", "tp"),
        P("sp", "tp"),
        P("sp", "tp"),
        P("sp", "tp"),
        P("sp", "tp"),
        P("sp", "tp"),
        P("sp", "tp"),
        P("tp", None),
        P("tp", None),
        P(),
        P("sp", "tp"),
        P("sp", "tp"),
        P(None, "tp"),
        P(None, "tp"),
        P("tp", "sp"),
    )
    out_specs = P(("sp", "tp"), None)
    return jax.shard_map(local, mesh=mesh, in_specs=in_specs, out_specs=out_specs, check_vma=False)
```

```python
import functools

import jax
import jax.numpy as jnp
from jax import lax
from jax.experimental import pallas as pl
from jax.experimental.pallas import tpu as pltpu
from jax.sharding import PartitionSpec as P

BLOCK = 128


eps = 1e-06
neg_large = -1e30


def shifted(x, axis, by):
    count = lax.axis_size(axis)
    pairs = [(i, i + by) for i in range(count) if 0 <= i + by < count]
    return lax.ppermute(x, axis, pairs)


def gate_log_values(input_gate_logits, forget_gate_logits, forget_decay_offset):
    input_log_value = 15.0 * jnp.tanh(input_gate_logits / 15.0)
    forget_log_sigmoid = (
        jax.nn.log_sigmoid(15.0 * jnp.tanh(forget_gate_logits / 15.0)) + forget_decay_offset
    )
    return (input_log_value, forget_log_sigmoid)


STATE_PAD = 16
MESH = pl.DeviceIdType.MESH


def cell_kernel(
    count,
    heads,
    state_ref,
    q_ref,
    k_ref,
    v_ref,
    gate_ref,
    gain_ref,
    rows_ref,
    cols_ref,
    out_ref,
    held,
    memory,
    normer,
    running,
    send_sem,
    recv_sem,
):
    me = lax.axis_index("sp")
    barrier = pltpu.get_barrier_semaphore()
    for d in range(1, count):
        pl.semaphore_signal(
            barrier, inc=1, device_id={"sp": lax.rem(me + d, count)}, device_id_type=MESH
        )
    pl.semaphore_wait(barrier, count - 1)

    def push(d, target, slot):
        return pltpu.make_async_remote_copy(
            src_ref=state_ref,
            dst_ref=held.at[slot],
            send_sem=send_sem.at[d],
            recv_sem=recv_sem.at[d],
            device_id={"sp": target},
            device_id_type=MESH,
        )

    for d in range(1, count):

        @pl.when(me + d < count)
        def _():
            push(d, me + d, me).start()

    memory[...] = jnp.zeros_like(memory)
    normer[...] = jnp.zeros_like(normer)
    running[...] = jnp.full(running.shape, neg_large, jnp.float32)
    for d in range(1, count):

        @pl.when(me - d >= 0)
        def _():
            push(d, lax.rem(me + d, count), me - d).wait_recv()

    key_width = memory.shape[1]
    value_width = memory.shape[2]
    span = key_width + STATE_PAD

    @pl.loop(0, me)
    def _(j):
        for h in range(heads):
            low = h * span
            extra = held[j, low + key_width : low + span, :].astype(jnp.float32)
            total = extra[2:3, :1] + extra[3:4, :1]
            level = extra[4:5, :1] + extra[5:6, :1]
            before = running[h, :1, :1]
            after = jnp.maximum(total + before, level)
            one = jnp.exp(total + before - after)
            two = jnp.exp(level - after)
            memory[h] = one * memory[h] + two * held[j, low : low + key_width, :].astype(
                jnp.float32
            )
            parts = extra[0:1, :key_width] + extra[1:2, :key_width]
            normer[h, :1, :] = one * normer[h, :1, :] + two * parts
            running[h] = jnp.broadcast_to(after, running.shape[1:])

    length = BLOCK
    scale = key_width ** (-0.5)
    at_row = lax.broadcasted_iota(jnp.int32, (length, length), 0)
    at_col = lax.broadcasted_iota(jnp.int32, (length, length), 1)
    causal = at_col <= at_row

    @pl.loop(0, q_ref.shape[0] // length)
    def _(j):
        rows = pl.ds(pl.multiple_of(j * length, length), length)
        lanes = rows_ref[j]
        cols = cols_ref[rows, :]
        for h in range(heads):
            keys = slice(h * key_width, (h + 1) * key_width)
            vals = slice(h * value_width, (h + 1) * value_width)
            q = q_ref[rows, keys]
            k = k_ref[rows, keys]
            v = v_ref[rows, vals]
            before = running[h, :1, :1]
            total = lanes[heads + h : heads + h + 1, :1]
            shifted_log = jnp.where(causal, lanes[h : h + 1, :], -jnp.inf)
            top = jnp.maximum(jnp.max(shifted_log, axis=1, keepdims=True), before)
            raw = (
                lax.dot_general(
                    q, k, (((1,), (1,)), ((), ())), preferred_element_type=jnp.float32
                )
                * scale
            )
            scores = raw * jnp.exp(shifted_log - top)
            carry = jnp.exp(before - top) * scale
            state = memory[h]
            high = state.astype(jnp.bfloat16)
            low = (state - high.astype(jnp.float32)).astype(jnp.bfloat16)
            carried = jnp.dot(q, high, preferred_element_type=jnp.float32) + jnp.dot(
                q, low, preferred_element_type=jnp.float32
            )
            numerator = carry * carried + jnp.dot(
                scores.astype(jnp.bfloat16), v, preferred_element_type=jnp.float32
            )
            denominator = carry * jnp.sum(
                q.astype(jnp.float32) * normer[h, :1, :], axis=1, keepdims=True
            ) + jnp.sum(scores, axis=1, keepdims=True)
            level = cols[:, h : h + 1] + top
            value = numerator / jnp.maximum(jnp.abs(denominator), jnp.exp(-level))
            mean = jnp.mean(value * value, axis=1, keepdims=True)
            normed = value * lax.rsqrt(mean + eps) * gain_ref[h : h + 1, :]
            gated = normed * jax.nn.sigmoid(gate_ref[rows, vals].astype(jnp.float32))
            out_ref[rows, vals] = gated.astype(out_ref.dtype)
            last = jnp.max(jnp.maximum(lanes[h : h + 1, :], before), axis=1, keepdims=True)
            decay = jnp.exp(before - last)
            weighted = k.astype(jnp.float32) * jnp.exp(cols[:, heads + h : heads + h + 1] - last)
            memory[h] = decay * state + lax.dot_general(
                weighted.astype(jnp.bfloat16),
                v,
                (((0,), (0,)), ((), ())),
                preferred_element_type=jnp.float32,
            )
            normer[h, :1, :] = decay * normer[h, :1, :] + jnp.sum(
                weighted, axis=0, keepdims=True
            )
            running[h] = jnp.broadcast_to(last + total, running.shape[1:])

    for d in range(1, count):

        @pl.when(me + d < count)
        def _():
            push(d, me + d, me).wait_send()


def halves(x):
    high = lax.reduce_precision(x, 8, 7)
    return (high.astype(jnp.bfloat16), (x - high).astype(jnp.bfloat16))


def cell(q, k, v, gates, input_log, forget_log, gain):
    heads = input_log.shape[1]
    tokens = q.shape[0]
    key_width = q.shape[1] // heads
    value_width = v.shape[1] // heads
    count = lax.axis_size("sp")
    blocks = tokens // BLOCK
    f = forget_log.reshape(blocks, BLOCK, heads)
    tri = jnp.tril(jnp.ones((BLOCK, BLOCK), jnp.float32))
    within = jnp.einsum("ts,bsh->bth", tri, f, precision=lax.Precision.HIGHEST)
    each = within[:, -1, :]
    later = jnp.triu(jnp.ones((blocks, blocks), jnp.float32), 1)
    after = jnp.einsum("bc,ch->bh", later, each, precision=lax.Precision.HIGHEST)
    total = jnp.sum(each, axis=0)
    shifted_log = input_log.reshape(blocks, BLOCK, heads) - within
    to_end = (shifted_log + (each + after)[:, None, :]).reshape(tokens, heads)
    level = jnp.max(to_end, axis=0)
    weighted = k.reshape(tokens, heads, key_width).astype(jnp.float32) * jnp.exp(to_end - level)[
        :, :, None
    ]
    memory = jnp.einsum(
        "shd,shv->hdv",
        weighted.astype(jnp.bfloat16),
        v.reshape(tokens, heads, value_width),
        preferred_element_type=jnp.float32,
    ).astype(jnp.bfloat16)
    normer = jnp.sum(weighted, axis=0)
    wide = (heads, 1, value_width)
    lines = [
        jnp.pad(part, ((0, 0), (0, value_width - key_width)))[:, None, :]
        for part in halves(normer)
    ]
    for scalar in (total, level):
        lines += [jnp.broadcast_to(part[:, None, None], wide) for part in halves(scalar)]
    lines.append(jnp.zeros((heads, STATE_PAD - len(lines), value_width), jnp.bfloat16))
    span = key_width + STATE_PAD
    state = jnp.concatenate([memory] + lines, axis=1).reshape(heads * span, value_width)
    lanes = jnp.concatenate(
        [
            jnp.transpose(shifted_log, (0, 2, 1)),
            jnp.broadcast_to(each[:, :, None], (blocks, heads, BLOCK)),
        ],
        axis=1,
    )
    cols = jnp.concatenate([within, shifted_log], axis=2).reshape(tokens, 2 * heads)
    vmem = pl.BlockSpec(memory_space=pltpu.VMEM)
    return pl.pallas_call(
        functools.partial(cell_kernel, count, heads),
        out_shape=jax.ShapeDtypeStruct(v.shape, jnp.bfloat16),
        in_specs=[vmem] * 8,
        out_specs=vmem,
        scratch_shapes=[
            pltpu.VMEM((count, heads * span, value_width), jnp.bfloat16),
            pltpu.VMEM((heads, key_width, value_width), jnp.float32),
            pltpu.VMEM((heads, 8, key_width), jnp.float32),
            pltpu.VMEM((heads, 8, 128), jnp.float32),
            pltpu.SemaphoreType.DMA((count,)),
            pltpu.SemaphoreType.DMA((count,)),
        ],
        compiler_params=pltpu.CompilerParams(
            collective_id=0, has_side_effects=True, vmem_limit_bytes=40 * 1024 * 1024
        ),
        cost_estimate=pl.CostEstimate(
            flops=30_000_000_000, bytes_accessed=8 * v.size, transcendentals=0
        ),
    )(state, q, k, v, gates, gain, lanes, cols)


def rows_kernel(pieces, x_ref, out_ref, own_sem, near_send, near_recv, far_send, far_recv, on_send, on_recv):
    me = lax.axis_index("tp")
    near = me + 1 - 2 * lax.rem(me, 2)
    far = lax.rem(me + 2, 4)
    opposite = lax.rem(near + 2, 4)
    size = x_ref.shape[0]
    step = size // pieces
    barrier = pltpu.get_barrier_semaphore()
    for other in (near, far):
        pl.semaphore_signal(barrier, inc=1, device_id={"tp": other}, device_id_type=MESH)
    pl.semaphore_wait(barrier, 2)

    def at(owner, p):
        return out_ref.at[pl.ds(pl.multiple_of(owner * size + p * step, step), step)]

    def send(src, dst, sems, p, target):
        return pltpu.make_async_remote_copy(
            src_ref=src,
            dst_ref=dst,
            send_sem=sems[0].at[p],
            recv_sem=sems[1].at[p],
            device_id={"tp": target},
            device_id_type=MESH,
        )

    mine = [x_ref.at[pl.ds(p * step, step)] for p in range(pieces)]
    far_out = [send(mine[p], at(me, p), (far_send, far_recv), p, far) for p in range(pieces)]
    near_out = [send(mine[p], at(me, p), (near_send, near_recv), p, near) for p in range(pieces)]
    far_in = [send(mine[p], at(far, p), (far_send, far_recv), p, far) for p in range(pieces)]
    near_in = [send(mine[p], at(near, p), (near_send, near_recv), p, near) for p in range(pieces)]
    onward = [send(at(far, p), at(far, p), (on_send, on_recv), p, near) for p in range(pieces)]
    on_in = [
        send(at(opposite, p), at(opposite, p), (on_send, on_recv), p, near)
        for p in range(pieces)
    ]
    for p in range(pieces):
        far_out[p].start()
    for p in range(pieces):
        near_out[p].start()
    whole = pl.ds(pl.multiple_of(me * size, size), size)
    own = pltpu.make_async_copy(x_ref, out_ref.at[whole], own_sem)
    own.start()
    for p in range(pieces):
        far_in[p].wait_recv()
        onward[p].start()
    own.wait()
    for p in range(pieces):
        near_in[p].wait_recv()
        on_in[p].wait_recv()
    for p in range(pieces):
        far_out[p].wait_send()
        near_out[p].wait_send()
        onward[p].wait_send()


def gather_rows(x):
    if lax.axis_size("tp") != 4:
        return lax.all_gather(x, "tp", axis=0, tiled=True)
    pieces = 4
    vmem = pl.BlockSpec(memory_space=pltpu.VMEM)
    return pl.pallas_call(
        functools.partial(rows_kernel, pieces),
        out_shape=jax.ShapeDtypeStruct((4 * x.shape[0], x.shape[1]), x.dtype),
        in_specs=[vmem],
        out_specs=vmem,
        scratch_shapes=[pltpu.SemaphoreType.DMA] + [pltpu.SemaphoreType.DMA((pieces,))] * 6,
        compiler_params=pltpu.CompilerParams(
            collective_id=1, has_side_effects=True, vmem_limit_bytes=16 * 1024 * 1024
        ),
        cost_estimate=pl.CostEstimate(
            flops=30_000_000_000, bytes_accessed=4 * x.size, transcendentals=0
        ),
    )(x)


def product_kernel(
    pieces,
    x_ref,
    w_ref,
    out_ref,
    pair_out,
    pair_in,
    far_out,
    far_in,
    near_out,
    near_in,
    pair_send,
    pair_recv,
    far_send,
    far_recv,
    near_send,
    near_recv,
):
    me = lax.axis_index("tp")
    near = me + 1 - 2 * lax.rem(me, 2)
    far = lax.rem(me + 2, 4)
    opposite = lax.rem(near + 2, 4)
    size = out_ref.shape[0]
    step = out_ref.shape[1] // pieces
    barrier = pltpu.get_barrier_semaphore()
    for other in (near, far):
        pl.semaphore_signal(barrier, inc=1, device_id={"tp": other}, device_id_type=MESH)
    pl.semaphore_wait(barrier, 2)

    def columns(p):
        return pl.ds(pl.multiple_of(p * step, step), step)

    def term(owner, p):
        rows = pl.ds(pl.multiple_of(owner * size, size), size)
        return jnp.dot(x_ref[rows, :], w_ref[:, columns(p)], preferred_element_type=jnp.float32)

    def send(src, dst, sems, p, target):
        return pltpu.make_async_remote_copy(
            src_ref=src.at[p],
            dst_ref=dst.at[p],
            send_sem=sems[0].at[p],
            recv_sem=sems[1].at[p],
            device_id={"tp": target},
            device_id_type=MESH,
        )

    def pair(p):
        return send(pair_out, pair_in, (pair_send, pair_recv), p, near)

    def across(p):
        return send(far_out, far_in, (far_send, far_recv), p, far)

    def beside(p):
        return send(near_out, near_in, (near_send, near_recv), p, near)

    @pl.loop(0, pieces)
    def _(p):
        pair_out[p] = term(opposite, p).astype(jnp.bfloat16)
        pair(p).start()
        mine = term(far, p)
        pair(p).wait_recv()
        far_out[p] = (mine + pair_in[p].astype(jnp.float32)).astype(jnp.bfloat16)
        across(p).start()

    @pl.loop(0, pieces)
    def _(p):
        near_out[p] = term(near, p).astype(jnp.bfloat16)
        beside(p).start()

    @pl.loop(0, pieces)
    def _(p):
        own = term(me, p)
        beside(p).wait_recv()
        out_ref[:, columns(p)] = own + near_in[p].astype(jnp.float32)

    @pl.loop(0, pieces)
    def _(p):
        across(p).wait_recv()
        out_ref[:, columns(p)] += far_in[p].astype(jnp.float32)

    @pl.loop(0, pieces)
    def _(p):
        pair(p).wait_send()
        across(p).wait_send()
        beside(p).wait_send()


def product_rows(x, w, tag):
    if lax.axis_size("tp") != 4:
        partial = jnp.dot(x, w, preferred_element_type=jnp.float32).astype(jnp.bfloat16)
        return lax.psum_scatter(partial, "tp", scatter_dimension=0, tiled=True).astype(
            jnp.float32
        )
    pieces = 4
    rows, wide = x.shape[0] // 4, w.shape[1]
    vmem = pl.BlockSpec(memory_space=pltpu.VMEM)
    slots = pltpu.VMEM((pieces, rows, wide // pieces), jnp.bfloat16)
    return pl.pallas_call(
        functools.partial(product_kernel, pieces),
        out_shape=jax.ShapeDtypeStruct((rows, wide), jnp.float32),
        in_specs=[vmem] * 2,
        out_specs=vmem,
        scratch_shapes=[slots] * 6 + [pltpu.SemaphoreType.DMA((pieces,))] * 6,
        compiler_params=pltpu.CompilerParams(
            collective_id=tag, has_side_effects=True, vmem_limit_bytes=40 * 1024 * 1024
        ),
        cost_estimate=pl.CostEstimate(
            flops=30_000_000_000, bytes_accessed=2 * w.size, transcendentals=0
        ),
    )(x, w)


def local(
    residual_entry_input,
    query_matrix_rows,
    key_matrix_rows,
    value_matrix_rows,
    output_gate_logits,
    input_gate_logits,
    forget_gate_logits,
    forget_decay_offset,
    head_norm_gain,
    cell_output_weight,
    feedforward_norm_gain,
    gate_up_weight,
    value_up_weight,
    gate_filter_taps,
    value_filter_taps,
    down_projection_weight,
):
    input_log, forget_log = gate_log_values(
        input_gate_logits, forget_gate_logits, forget_decay_offset
    )
    whole_gate = lax.all_gather(gate_up_weight, "sp", axis=0, tiled=True)
    whole_value = lax.all_gather(value_up_weight, "sp", axis=0, tiled=True)
    whole_down = lax.all_gather(down_projection_weight, "sp", axis=1, tiled=True)
    gated_rows = cell(
        query_matrix_rows,
        key_matrix_rows,
        value_matrix_rows,
        output_gate_logits,
        input_log,
        forget_log,
        head_norm_gain,
    )
    mixed_rows = product_rows(gated_rows, cell_output_weight, 2)
    stream_wide = residual_entry_input.astype(jnp.float32) + mixed_rows
    stream = stream_wide.astype(jnp.bfloat16)
    stream_wide = lax.optimization_barrier(stream).astype(jnp.float32)
    normed_rows = (
        stream_wide
        * lax.rsqrt(jnp.mean(stream_wide * stream_wide, axis=-1, keepdims=True) + eps)
        * feedforward_norm_gain[None, :]
    ).astype(jnp.bfloat16)
    group_rows = gather_rows(normed_rows)
    earlier_rows = shifted(group_rows[-2:], "sp", 1)
    window = jnp.concatenate([earlier_rows, group_rows], axis=0)
    up_gate = jnp.dot(
        window,
        whole_gate,
        preferred_element_type=jnp.float32,
    )
    up_value = jnp.dot(
        window,
        whole_value,
        preferred_element_type=jnp.float32,
    )
    conv_g = (
        gate_filter_taps[0][None, :] * up_gate[:-2]
        + gate_filter_taps[1][None, :] * up_gate[1:-1]
        + gate_filter_taps[2][None, :] * up_gate[2:]
    )
    conv_v = (
        value_filter_taps[0][None, :] * up_value[:-2]
        + value_filter_taps[1][None, :] * up_value[1:-1]
        + value_filter_taps[2][None, :] * up_value[2:]
    )
    hidden = (jax.nn.silu(conv_g) * conv_v).astype(jnp.bfloat16)
    ffn_rows = product_rows(hidden, whole_down, 3)
    return (stream_wide + ffn_rows).astype(jnp.bfloat16)


def solution(mesh):
    in_specs = (
        P(("sp", "tp"), None),
        P("sp", "tp"),
        P("sp", "tp"),
        P("sp", "tp"),
        P("sp", "tp"),
        P("sp", "tp"),
        P("sp", "tp"),
        P("sp", "tp"),
        P("tp", None),
        P("tp", None),
        P(),
        P("sp", "tp"),
        P("sp", "tp"),
        P(None, "tp"),
        P(None, "tp"),
        P("tp", "sp"),
    )
    out_specs = P(("sp", "tp"), None)
    return jax.shard_map(local, mesh=mesh, in_specs=in_specs, out_specs=out_specs, check_vma=False)
```

```python
import functools

import jax
import jax.numpy as jnp
from jax import lax
from jax.experimental import pallas as pl
from jax.experimental.pallas import tpu as pltpu
from jax.sharding import PartitionSpec as P

BLOCK = 128


eps = 1e-06
neg_large = -1e30


def shifted(x, axis, by):
    count = lax.axis_size(axis)
    pairs = [(i, i + by) for i in range(count) if 0 <= i + by < count]
    return lax.ppermute(x, axis, pairs)


def gate_log_values(input_gate_logits, forget_gate_logits, forget_decay_offset):
    input_log_value = 15.0 * jnp.tanh(input_gate_logits / 15.0)
    forget_log_sigmoid = (
        jax.nn.log_sigmoid(15.0 * jnp.tanh(forget_gate_logits / 15.0)) + forget_decay_offset
    )
    return (input_log_value, forget_log_sigmoid)


STATE_PAD = 16
MESH = pl.DeviceIdType.MESH


def cell_kernel(
    count,
    heads,
    state_ref,
    q_ref,
    k_ref,
    v_ref,
    gate_ref,
    gain_ref,
    rows_ref,
    cols_ref,
    out_ref,
    held,
    memory,
    normer,
    running,
    send_sem,
    recv_sem,
):
    me = lax.axis_index("sp")
    barrier = pltpu.get_barrier_semaphore()
    for d in range(1, count):
        pl.semaphore_signal(
            barrier, inc=1, device_id={"sp": lax.rem(me + d, count)}, device_id_type=MESH
        )
    pl.semaphore_wait(barrier, count - 1)

    def push(d, target, slot):
        return pltpu.make_async_remote_copy(
            src_ref=state_ref,
            dst_ref=held.at[slot],
            send_sem=send_sem.at[d],
            recv_sem=recv_sem.at[d],
            device_id={"sp": target},
            device_id_type=MESH,
        )

    for d in range(1, count):

        @pl.when(me + d < count)
        def _():
            push(d, me + d, me).start()

    memory[...] = jnp.zeros_like(memory)
    normer[...] = jnp.zeros_like(normer)
    running[...] = jnp.full(running.shape, neg_large, jnp.float32)
    for d in range(1, count):

        @pl.when(me - d >= 0)
        def _():
            push(d, lax.rem(me + d, count), me - d).wait_recv()

    key_width = memory.shape[1]
    value_width = memory.shape[2]
    span = key_width + STATE_PAD

    @pl.loop(0, me)
    def _(j):
        for h in range(heads):
            low = h * span
            extra = held[j, low + key_width : low + span, :].astype(jnp.float32)
            total = extra[2:3, :1] + extra[3:4, :1]
            level = extra[4:5, :1] + extra[5:6, :1]
            before = running[h, :1, :1]
            after = jnp.maximum(total + before, level)
            one = jnp.exp(total + before - after)
            two = jnp.exp(level - after)
            memory[h] = one * memory[h] + two * held[j, low : low + key_width, :].astype(
                jnp.float32
            )
            parts = extra[0:1, :key_width] + extra[1:2, :key_width]
            normer[h, :1, :] = one * normer[h, :1, :] + two * parts
            running[h] = jnp.broadcast_to(after, running.shape[1:])

    length = BLOCK
    scale = key_width ** (-0.5)
    at_row = lax.broadcasted_iota(jnp.int32, (length, length), 0)
    at_col = lax.broadcasted_iota(jnp.int32, (length, length), 1)
    causal = at_col <= at_row

    @pl.loop(0, q_ref.shape[0] // length)
    def _(j):
        rows = pl.ds(pl.multiple_of(j * length, length), length)
        lanes = rows_ref[j]
        cols = cols_ref[rows, :]
        for h in range(heads):
            keys = slice(h * key_width, (h + 1) * key_width)
            vals = slice(h * value_width, (h + 1) * value_width)
            q = q_ref[rows, keys]
            k = k_ref[rows, keys]
            v = v_ref[rows, vals]
            before = running[h, :1, :1]
            total = lanes[heads + h : heads + h + 1, :1]
            shifted_log = jnp.where(causal, lanes[h : h + 1, :], -jnp.inf)
            top = jnp.maximum(jnp.max(shifted_log, axis=1, keepdims=True), before)
            raw = (
                lax.dot_general(
                    q, k, (((1,), (1,)), ((), ())), preferred_element_type=jnp.float32
                )
                * scale
            )
            scores = raw * jnp.exp(shifted_log - top)
            carry = jnp.exp(before - top) * scale
            state = memory[h]
            high = state.astype(jnp.bfloat16)
            low = (state - high.astype(jnp.float32)).astype(jnp.bfloat16)
            carried = jnp.dot(q, high, preferred_element_type=jnp.float32) + jnp.dot(
                q, low, preferred_element_type=jnp.float32
            )
            numerator = carry * carried + jnp.dot(
                scores.astype(jnp.bfloat16), v, preferred_element_type=jnp.float32
            )
            denominator = carry * jnp.sum(
                q.astype(jnp.float32) * normer[h, :1, :], axis=1, keepdims=True
            ) + jnp.sum(scores, axis=1, keepdims=True)
            level = cols[:, h : h + 1] + top
            value = numerator / jnp.maximum(jnp.abs(denominator), jnp.exp(-level))
            mean = jnp.mean(value * value, axis=1, keepdims=True)
            normed = value * lax.rsqrt(mean + eps) * gain_ref[h : h + 1, :]
            gated = normed * jax.nn.sigmoid(gate_ref[rows, vals].astype(jnp.float32))
            out_ref[rows, vals] = gated.astype(out_ref.dtype)
            last = jnp.max(jnp.maximum(lanes[h : h + 1, :], before), axis=1, keepdims=True)
            decay = jnp.exp(before - last)
            weighted = k.astype(jnp.float32) * jnp.exp(cols[:, heads + h : heads + h + 1] - last)
            memory[h] = decay * state + lax.dot_general(
                weighted.astype(jnp.bfloat16),
                v,
                (((0,), (0,)), ((), ())),
                preferred_element_type=jnp.float32,
            )
            normer[h, :1, :] = decay * normer[h, :1, :] + jnp.sum(
                weighted, axis=0, keepdims=True
            )
            running[h] = jnp.broadcast_to(last + total, running.shape[1:])

    for d in range(1, count):

        @pl.when(me + d < count)
        def _():
            push(d, me + d, me).wait_send()


def halves(x):
    high = lax.reduce_precision(x, 8, 7)
    return (high.astype(jnp.bfloat16), (x - high).astype(jnp.bfloat16))


def cell(q, k, v, gates, input_log, forget_log, gain):
    heads = input_log.shape[1]
    tokens = q.shape[0]
    key_width = q.shape[1] // heads
    value_width = v.shape[1] // heads
    count = lax.axis_size("sp")
    blocks = tokens // BLOCK
    f = forget_log.reshape(blocks, BLOCK, heads)
    tri = jnp.tril(jnp.ones((BLOCK, BLOCK), jnp.float32))
    within = jnp.einsum("ts,bsh->bth", tri, f, precision=lax.Precision.HIGHEST)
    each = within[:, -1, :]
    later = jnp.triu(jnp.ones((blocks, blocks), jnp.float32), 1)
    after = jnp.einsum("bc,ch->bh", later, each, precision=lax.Precision.HIGHEST)
    total = jnp.sum(each, axis=0)
    shifted_log = input_log.reshape(blocks, BLOCK, heads) - within
    to_end = (shifted_log + (each + after)[:, None, :]).reshape(tokens, heads)
    level = jnp.max(to_end, axis=0)
    weighted = k.reshape(tokens, heads, key_width).astype(jnp.float32) * jnp.exp(to_end - level)[
        :, :, None
    ]
    memory = jnp.einsum(
        "shd,shv->hdv",
        weighted.astype(jnp.bfloat16),
        v.reshape(tokens, heads, value_width),
        preferred_element_type=jnp.float32,
    ).astype(jnp.bfloat16)
    normer = jnp.sum(weighted, axis=0)
    wide = (heads, 1, value_width)
    lines = [
        jnp.pad(part, ((0, 0), (0, value_width - key_width)))[:, None, :]
        for part in halves(normer)
    ]
    for scalar in (total, level):
        lines += [jnp.broadcast_to(part[:, None, None], wide) for part in halves(scalar)]
    lines.append(jnp.zeros((heads, STATE_PAD - len(lines), value_width), jnp.bfloat16))
    span = key_width + STATE_PAD
    state = jnp.concatenate([memory] + lines, axis=1).reshape(heads * span, value_width)
    lanes = jnp.concatenate(
        [
            jnp.transpose(shifted_log, (0, 2, 1)),
            jnp.broadcast_to(each[:, :, None], (blocks, heads, BLOCK)),
        ],
        axis=1,
    )
    cols = jnp.concatenate([within, shifted_log], axis=2).reshape(tokens, 2 * heads)
    vmem = pl.BlockSpec(memory_space=pltpu.VMEM)
    return pl.pallas_call(
        functools.partial(cell_kernel, count, heads),
        out_shape=jax.ShapeDtypeStruct(v.shape, jnp.bfloat16),
        in_specs=[vmem] * 8,
        out_specs=vmem,
        scratch_shapes=[
            pltpu.VMEM((count, heads * span, value_width), jnp.bfloat16),
            pltpu.VMEM((heads, key_width, value_width), jnp.float32),
            pltpu.VMEM((heads, 8, key_width), jnp.float32),
            pltpu.VMEM((heads, 8, 128), jnp.float32),
            pltpu.SemaphoreType.DMA((count,)),
            pltpu.SemaphoreType.DMA((count,)),
        ],
        compiler_params=pltpu.CompilerParams(
            collective_id=0, has_side_effects=True, vmem_limit_bytes=40 * 1024 * 1024
        ),
        cost_estimate=pl.CostEstimate(
            flops=30_000_000_000, bytes_accessed=8 * v.size, transcendentals=0
        ),
    )(state, q, k, v, gates, gain, lanes, cols)


def rows_kernel(pieces, x_ref, out_ref, own_sem, near_send, near_recv, far_send, far_recv, on_send, on_recv):
    me = lax.axis_index("tp")
    near = me + 1 - 2 * lax.rem(me, 2)
    far = lax.rem(me + 2, 4)
    opposite = lax.rem(near + 2, 4)
    size = x_ref.shape[0]
    step = size // pieces
    barrier = pltpu.get_barrier_semaphore()
    for other in (near, far):
        pl.semaphore_signal(barrier, inc=1, device_id={"tp": other}, device_id_type=MESH)
    pl.semaphore_wait(barrier, 2)

    def at(owner, p):
        return out_ref.at[pl.ds(pl.multiple_of(owner * size + p * step, step), step)]

    def send(src, dst, sems, p, target):
        return pltpu.make_async_remote_copy(
            src_ref=src,
            dst_ref=dst,
            send_sem=sems[0].at[p],
            recv_sem=sems[1].at[p],
            device_id={"tp": target},
            device_id_type=MESH,
        )

    mine = [x_ref.at[pl.ds(p * step, step)] for p in range(pieces)]
    far_out = [send(mine[p], at(me, p), (far_send, far_recv), p, far) for p in range(pieces)]
    near_out = [send(mine[p], at(me, p), (near_send, near_recv), p, near) for p in range(pieces)]
    far_in = [send(mine[p], at(far, p), (far_send, far_recv), p, far) for p in range(pieces)]
    near_in = [send(mine[p], at(near, p), (near_send, near_recv), p, near) for p in range(pieces)]
    onward = [send(at(far, p), at(far, p), (on_send, on_recv), p, near) for p in range(pieces)]
    on_in = [
        send(at(opposite, p), at(opposite, p), (on_send, on_recv), p, near)
        for p in range(pieces)
    ]
    for p in range(pieces):
        far_out[p].start()
    for p in range(pieces):
        near_out[p].start()
    whole = pl.ds(pl.multiple_of(me * size, size), size)
    own = pltpu.make_async_copy(x_ref, out_ref.at[whole], own_sem)
    own.start()
    for p in range(pieces):
        far_in[p].wait_recv()
        onward[p].start()
    own.wait()
    for p in range(pieces):
        near_in[p].wait_recv()
        on_in[p].wait_recv()
    for p in range(pieces):
        far_out[p].wait_send()
        near_out[p].wait_send()
        onward[p].wait_send()


def gather_rows(x):
    if lax.axis_size("tp") != 4:
        return lax.all_gather(x, "tp", axis=0, tiled=True)
    pieces = 4
    vmem = pl.BlockSpec(memory_space=pltpu.VMEM)
    return pl.pallas_call(
        functools.partial(rows_kernel, pieces),
        out_shape=jax.ShapeDtypeStruct((4 * x.shape[0], x.shape[1]), x.dtype),
        in_specs=[vmem],
        out_specs=vmem,
        scratch_shapes=[pltpu.SemaphoreType.DMA] + [pltpu.SemaphoreType.DMA((pieces,))] * 6,
        compiler_params=pltpu.CompilerParams(
            collective_id=1, has_side_effects=True, vmem_limit_bytes=16 * 1024 * 1024
        ),
        cost_estimate=pl.CostEstimate(
            flops=30_000_000_000, bytes_accessed=4 * x.size, transcendentals=0
        ),
    )(x)


def product_kernel(
    pieces,
    x_ref,
    w_ref,
    out_ref,
    pair_out,
    pair_in,
    far_out,
    far_in,
    near_out,
    near_in,
    pair_send,
    pair_recv,
    far_send,
    far_recv,
    near_send,
    near_recv,
):
    me = lax.axis_index("tp")
    near = me + 1 - 2 * lax.rem(me, 2)
    far = lax.rem(me + 2, 4)
    opposite = lax.rem(near + 2, 4)
    size = out_ref.shape[0]
    step = out_ref.shape[1] // pieces
    barrier = pltpu.get_barrier_semaphore()
    for other in (near, far):
        pl.semaphore_signal(barrier, inc=1, device_id={"tp": other}, device_id_type=MESH)
    pl.semaphore_wait(barrier, 2)

    def columns(p):
        return pl.ds(pl.multiple_of(p * step, step), step)

    def term(owner, p):
        rows = pl.ds(pl.multiple_of(owner * size, size), size)
        return jnp.dot(x_ref[rows, :], w_ref[:, columns(p)], preferred_element_type=jnp.float32)

    def send(src, dst, sems, p, target):
        return pltpu.make_async_remote_copy(
            src_ref=src.at[p],
            dst_ref=dst.at[p],
            send_sem=sems[0].at[p],
            recv_sem=sems[1].at[p],
            device_id={"tp": target},
            device_id_type=MESH,
        )

    def pair(p):
        return send(pair_out, pair_in, (pair_send, pair_recv), p, near)

    def across(p):
        return send(far_out, far_in, (far_send, far_recv), p, far)

    def beside(p):
        return send(near_out, near_in, (near_send, near_recv), p, near)

    @pl.loop(0, pieces)
    def _(p):
        pair_out[p] = term(opposite, p).astype(jnp.bfloat16)
        pair(p).start()
        mine = term(far, p)
        pair(p).wait_recv()
        far_out[p] = (mine + pair_in[p].astype(jnp.float32)).astype(jnp.bfloat16)
        across(p).start()

    @pl.loop(0, pieces)
    def _(p):
        near_out[p] = term(near, p).astype(jnp.bfloat16)
        beside(p).start()

    @pl.loop(0, pieces)
    def _(p):
        own = term(me, p)
        beside(p).wait_recv()
        out_ref[:, columns(p)] = own + near_in[p].astype(jnp.float32)

    @pl.loop(0, pieces)
    def _(p):
        across(p).wait_recv()
        out_ref[:, columns(p)] += far_in[p].astype(jnp.float32)

    @pl.loop(0, pieces)
    def _(p):
        pair(p).wait_send()
        across(p).wait_send()
        beside(p).wait_send()


def product_rows(x, w, tag):
    if lax.axis_size("tp") != 4:
        partial = jnp.dot(x, w, preferred_element_type=jnp.float32).astype(jnp.bfloat16)
        return lax.psum_scatter(partial, "tp", scatter_dimension=0, tiled=True).astype(
            jnp.float32
        )
    pieces = 4
    rows, wide = x.shape[0] // 4, w.shape[1]
    vmem = pl.BlockSpec(memory_space=pltpu.VMEM)
    slots = pltpu.VMEM((pieces, rows, wide // pieces), jnp.bfloat16)
    return pl.pallas_call(
        functools.partial(product_kernel, pieces),
        out_shape=jax.ShapeDtypeStruct((rows, wide), jnp.float32),
        in_specs=[vmem] * 2,
        out_specs=vmem,
        scratch_shapes=[slots] * 6 + [pltpu.SemaphoreType.DMA((pieces,))] * 6,
        compiler_params=pltpu.CompilerParams(
            collective_id=tag, has_side_effects=True, vmem_limit_bytes=40 * 1024 * 1024
        ),
        cost_estimate=pl.CostEstimate(
            flops=30_000_000_000, bytes_accessed=2 * w.size, transcendentals=0
        ),
    )(x, w)


def walk_kernel(count, pieces, x_ref, out_ref, own_sem, send_sem, recv_sem):
    me = lax.axis_index("sp")
    odd = lax.rem(me, 2)
    place = me // 2 + odd * (count - 1 - 2 * (me // 2))
    size = x_ref.shape[0]
    step = size // (2 * pieces)

    def index(position):
        position = lax.rem(position + 2 * count, count)
        back = position // (count // 2)
        return (1 - back) * 2 * position + back * (2 * (count - 1 - position) + 1)

    ways = (1, -1)
    barrier = pltpu.get_barrier_semaphore()
    for way in ways:
        pl.semaphore_signal(
            barrier, inc=1, device_id={"sp": index(place + way)}, device_id_type=MESH
        )
    pl.semaphore_wait(barrier, 2)

    def hop(w, t, p, age, own=False):
        inner = (w * pieces + p) * step
        owner = index(place - ways[w] * age)
        dst = out_ref.at[pl.ds(pl.multiple_of(owner * size + inner, step), step)]
        return pltpu.make_async_remote_copy(
            src_ref=x_ref.at[pl.ds(inner, step)] if own else dst,
            dst_ref=dst,
            send_sem=send_sem.at[w, p, t],
            recv_sem=recv_sem.at[w, p, t],
            device_id={"sp": index(place + ways[w])},
            device_id_type=MESH,
        )

    for p in range(pieces):
        for w in range(2):
            hop(w, 0, p, 0, True).start()
    whole = pl.ds(pl.multiple_of(me * size, size), size)
    own = pltpu.make_async_copy(x_ref, out_ref.at[whole], own_sem)
    own.start()

    @pl.loop(1, count - 1)
    def _(t):
        for p in range(pieces):
            for w in range(2):
                hop(w, t - 1, p, t).wait_recv()
                hop(w, t, p, t).start()

    own.wait()
    for p in range(pieces):
        for w in range(2):
            hop(w, count - 2, p, count - 1).wait_recv()
            hop(w, 0, p, 0, True).wait_send()

    @pl.loop(1, count - 1)
    def _(t):
        for p in range(pieces):
            for w in range(2):
                hop(w, t, p, t).wait_send()


def walk_gather(x, pieces):
    count = lax.axis_size("sp")
    if count % 2 or count < 4 or x.shape[0] % (32 * pieces):
        return lax.all_gather(x, "sp", axis=0, tiled=True)
    vmem = pl.BlockSpec(memory_space=pltpu.VMEM)
    return pl.pallas_call(
        functools.partial(walk_kernel, count, pieces),
        out_shape=jax.ShapeDtypeStruct((count * x.shape[0], x.shape[1]), x.dtype),
        in_specs=[vmem],
        out_specs=vmem,
        scratch_shapes=[pltpu.SemaphoreType.DMA]
        + [pltpu.SemaphoreType.DMA((2, pieces, count - 1))] * 2,
        compiler_params=pltpu.CompilerParams(
            collective_id=4, has_side_effects=True, vmem_limit_bytes=16 * 1024 * 1024
        ),
        cost_estimate=pl.CostEstimate(
            flops=30_000_000_000, bytes_accessed=count * x.size, transcendentals=0
        ),
    )(x)


def local(
    residual_entry_input,
    query_matrix_rows,
    key_matrix_rows,
    value_matrix_rows,
    output_gate_logits,
    input_gate_logits,
    forget_gate_logits,
    forget_decay_offset,
    head_norm_gain,
    cell_output_weight,
    feedforward_norm_gain,
    gate_up_weight,
    value_up_weight,
    gate_filter_taps,
    value_filter_taps,
    down_projection_weight,
):
    input_log, forget_log = gate_log_values(
        input_gate_logits, forget_gate_logits, forget_decay_offset
    )
    whole_gate = lax.all_gather(gate_up_weight, "sp", axis=0, tiled=True)
    whole_down = lax.all_gather(down_projection_weight, "sp", axis=1, tiled=True)
    gated_rows = cell(
        query_matrix_rows,
        key_matrix_rows,
        value_matrix_rows,
        output_gate_logits,
        input_log,
        forget_log,
        head_norm_gain,
    )
    mixed_rows = product_rows(gated_rows, cell_output_weight, 2)
    stream_wide = residual_entry_input.astype(jnp.float32) + mixed_rows
    stream = stream_wide.astype(jnp.bfloat16)
    stream_wide = lax.optimization_barrier(stream).astype(jnp.float32)
    normed_rows = (
        stream_wide
        * lax.rsqrt(jnp.mean(stream_wide * stream_wide, axis=-1, keepdims=True) + eps)
        * feedforward_norm_gain[None, :]
    ).astype(jnp.bfloat16)
    group_rows = gather_rows(normed_rows)
    group_rows, value_shard = lax.optimization_barrier((group_rows, value_up_weight))
    whole_value = walk_gather(value_shard, 2)
    earlier_rows = shifted(group_rows[-2:], "sp", 1)
    window = jnp.concatenate([earlier_rows, group_rows], axis=0)
    up_gate = jnp.dot(
        window,
        whole_gate,
        preferred_element_type=jnp.float32,
    )
    up_value = jnp.dot(
        window,
        whole_value,
        preferred_element_type=jnp.float32,
    )
    conv_g = (
        gate_filter_taps[0][None, :] * up_gate[:-2]
        + gate_filter_taps[1][None, :] * up_gate[1:-1]
        + gate_filter_taps[2][None, :] * up_gate[2:]
    )
    conv_v = (
        value_filter_taps[0][None, :] * up_value[:-2]
        + value_filter_taps[1][None, :] * up_value[1:-1]
        + value_filter_taps[2][None, :] * up_value[2:]
    )
    hidden = (jax.nn.silu(conv_g) * conv_v).astype(jnp.bfloat16)
    ffn_rows = product_rows(hidden, whole_down, 3)
    return (stream_wide + ffn_rows).astype(jnp.bfloat16)


def solution(mesh):
    in_specs = (
        P(("sp", "tp"), None),
        P("sp", "tp"),
        P("sp", "tp"),
        P("sp", "tp"),
        P("sp", "tp"),
        P("sp", "tp"),
        P("sp", "tp"),
        P("sp", "tp"),
        P("tp", None),
        P("tp", None),
        P(),
        P("sp", "tp"),
        P("sp", "tp"),
        P(None, "tp"),
        P(None, "tp"),
        P("tp", "sp"),
    )
    out_specs = P(("sp", "tp"), None)
    return jax.shard_map(local, mesh=mesh, in_specs=in_specs, out_specs=out_specs, check_vma=False)
```
